512 devices in a mesh: gr: 2 (over z_hi), fs: 32 (over z_lo, y), tp: 8 (over x, core).
Axes of the slice: x: 4, y: 8, z: 8 (z_hi: 2, z_lo: 4; z = z_hi * 4 + z_lo), core: 2. Of those that a mesh axis runs over, the one named last changes fastest.
Arguments:
- prompt: bfloat16 [20480, 2048], P(('gr', 'fs'), 'tp'), may hold values from -6 to 6
- norm_gain: float32 [2048], P(('gr', 'fs')), may hold values from 0.1 to 1.9
- gate_weight: float32 [32, 2048, 2048], P(None, ('gr', 'fs'), 'tp'), may hold values from -0.125 to 0.125
- up_weight: float32 [32, 2048, 2048], P(None, ('gr', 'fs'), 'tp'), may hold values from -0.125 to 0.125
- down_weight: float32 [32, 2048, 2048], P(None, ('gr', 'fs'), 'tp'), may hold values from -0.125 to 0.125
- routes: int32 [20480, 2], P(('gr', 'fs')), may hold values from 0 to 31, as said below
- route_weight: float32 [20480, 2], P(('gr', 'fs')), may hold values from 0.2 to 1
Outputs:
- gate_new: bfloat16 [32, 2048, 2048], P('fs', None, 'tp')
- up_new: bfloat16 [32, 2048, 2048], P('fs', None, 'tp')
- down_new: bfloat16 [32, 2048, 2048], P('fs', 'tp')
- mixed: bfloat16 [20480, 2048], P(('gr', 'fs'), 'tp')
The draws below stay inside these ranges and needn't reach their ends.
Inputs may be any that keep to these rules, and one draw needn't show every extreme that they name: `routes`: each row names two different experts of the same group; expert e belongs to group e // 8. Among the 320 rows of one index of gr and fs no expert is named more than 30 times, and in every draw every expert of one group is named exactly 30 times by the rows of every index.
All inputs are finite; a program needn't handle non-finite values.
Results may differ from the reference program's by a relative error of at most 0.015.
Values may be sent and summed in bfloat16 or wider, within the bound.
No kernel may reach another device: no remote copies, remote signals or barrier semaphores. Data moves between devices by JAX's collectives and lax.ppermute only.
A program may use at most 64 MiB of HBM per device.

```python
import jax
import jax.numpy as jnp
from jax import lax

D = 2048
FF = 2048
GROUPS = 4
EXP_GROUP = 8
TOK_DEV = 320
EXPERTS = 32
CAP = 30
TOKENS = 20480
N_GR = 2
N_FS = 32
N_TP = 8


def draw_routes(key, part):
    big_group = jax.random.randint(jax.random.fold_in(key, 101), (), 0, GROUPS)
    full = 4 * CAP
    rest = TOK_DEV - full
    spacing = rest // (GROUPS - 1)
    jitter = spacing // 4

    def one_source(source):
        source_key = jax.random.fold_in(key, source)
        key_rank, key_bound, key_shift = jax.random.split(source_key, 3)
        ranking = jax.random.permutation(key_rank, TOK_DEV).astype(jnp.int32)
        inner = jnp.arange(1, GROUPS - 1, dtype=jnp.int32) * rest // (GROUPS - 1)
        inner = inner + jax.random.randint(key_bound, (GROUPS - 2,), -jitter, jitter + 1)
        bounds = jnp.concatenate([jnp.zeros((1,), jnp.int32), inner.astype(jnp.int32)])
        remain = ranking - full
        slot_index = jnp.sum((remain[:, None] >= inner[None, :]).astype(jnp.int32), axis=1)
        in_big = ranking < full
        within = jnp.where(in_big, ranking, remain - bounds[slot_index])
        other = slot_index + (slot_index >= big_group).astype(jnp.int32)
        group_id = jnp.where(in_big, big_group, other)
        shifts = jax.random.randint(key_shift, (GROUPS,), 0, EXP_GROUP)
        offset = shifts[group_id]
        first = (within + offset) % EXP_GROUP
        second = (within + offset + 1 + within // EXP_GROUP % (EXP_GROUP - 1)) % EXP_GROUP
        return jnp.stack([group_id * EXP_GROUP + first, group_id * EXP_GROUP + second], axis=1)
    sources = jnp.arange(N_GR * N_FS, dtype=jnp.int32)
    return jax.vmap(one_source)(sources).reshape(TOKENS, 2).astype(jnp.int32)


def level_of(key, extent, shards, low, top_value):
    gain, own = 1.0, jax.random.fold_in(key, 6)
    for position, shards_of in shards:
        steps = jnp.exp(jax.random.uniform(jax.random.fold_in(own, position), (shards_of,), jnp.float32, low / len(shards), top_value / len(shards)))
        gain = gain * jnp.repeat(steps, extent[position] // shards_of).reshape([-1 if axis == position else 1 for axis in range(len(extent))])
    return gain


def normal_values(rng, shape, width, most, cuts=(), held_as=jnp.bfloat16):
    drawn = jax.random.normal(rng, shape, jnp.float32) * width
    if len(cuts) > 0:
        drawn = level_of(rng, shape, cuts, -0.22, 0.18) * drawn
    return jnp.clip(drawn, min=-most, max=most).astype(held_as)


def setup_inputs(seed: int = 0) -> dict:
    streams_of = jax.random.split(jax.random.key(seed), 8)
    return {
        "prompt": normal_values(streams_of[0], (TOKENS, D), 1.0, 6.0, ((0, 64), (1, 8))),
        "norm_gain": jnp.clip(1.0 + 0.18 * jax.random.normal(streams_of[1], (D,), jnp.float32), 0.1, 1.9),
        "gate_weight": normal_values(streams_of[2], (EXPERTS, D, FF), D ** -0.5, 0.125, ((1, 64), (2, 8)), jnp.float32),
        "up_weight": normal_values(streams_of[3], (EXPERTS, D, FF), D ** -0.5, 0.125, ((1, 64), (2, 8)), jnp.float32),
        "down_weight": normal_values(streams_of[4], (EXPERTS, FF, D), FF ** -0.5, 0.125, ((1, 64), (2, 8)), jnp.float32),
        "routes": draw_routes(jax.random.fold_in(streams_of[7], 71), 0),
        "route_weight": jnp.clip(0.2 + 0.8 * jax.random.uniform(streams_of[6], (TOKENS, 2), jnp.float32) ** level_of(streams_of[6], (TOKENS, 2), ((0, 64),), -0.2, 0.2), 0.2, 1.0),
    }


def reference(prompt, norm_gain, gate_weight, up_weight, down_weight, routes, route_weight):
    gate_new = (gate_weight * norm_gain[None, :, None]).astype(jnp.bfloat16)
    up_new = (up_weight * norm_gain[None, :, None]).astype(jnp.bfloat16)
    down_new = down_weight.astype(jnp.bfloat16)
    values = prompt.astype(jnp.float32)
    normed = (values * lax.rsqrt(lax.optimization_barrier(jnp.mean(values * values, axis=-1, keepdims=True)) + 1e-06)).astype(jnp.bfloat16)
    picks_flat = routes.reshape(-1)
    total = picks_flat.shape[0]
    most = N_GR * N_FS * CAP
    normed_pad = jnp.concatenate([normed, jnp.zeros((1, D), jnp.bfloat16)], axis=0)
    weight_pad = jnp.concatenate([route_weight.reshape(-1), jnp.zeros((1,), jnp.float32)], axis=0)

    def one_expert(accum, expert):
        chosen = jnp.nonzero(picks_flat == expert, size=most, fill_value=total)[0].astype(jnp.int32)
        tok_rows = (chosen // 2).astype(jnp.int32)
        arrived = normed_pad[tok_rows]
        gate_pre = jnp.dot(arrived, gate_new[expert], preferred_element_type=jnp.float32)
        up_pre = jnp.dot(arrived, up_new[expert], preferred_element_type=jnp.float32)
        hidden = (jax.nn.silu(gate_pre) * up_pre).astype(jnp.bfloat16)
        blocks = hidden.reshape(most, N_TP, FF // N_TP).astype(jnp.float32)
        down_blocks = down_new[expert].reshape(N_TP, FF // N_TP, D).astype(jnp.float32)
        partial_value = jnp.einsum('rkh,khd->rkd', blocks, down_blocks).astype(jnp.bfloat16)
        partial_value = lax.optimization_barrier(partial_value).astype(jnp.float32)
        expert_out = lax.optimization_barrier(jnp.sum(partial_value, axis=1)).astype(jnp.bfloat16)
        expert_out = lax.optimization_barrier(expert_out).astype(jnp.float32)
        accum = accum.at[tok_rows].add(expert_out * weight_pad[chosen][:, None])
        return (accum, None)
    start = jnp.zeros((TOKENS + 1, D), jnp.float32)
    accum, _ = lax.scan(one_expert, start, jnp.arange(EXPERTS, dtype=jnp.int32))
    mixed = accum[:TOKENS].astype(jnp.bfloat16)
    return (gate_new, up_new, down_new, mixed)
```

```python
import functools

import jax
import jax.numpy as jnp
from jax import lax
from jax.experimental import pallas as pl
from jax.experimental.pallas import tpu as pltpu
from jax.sharding import PartitionSpec as P

SLOTS = 32
BF = jnp.bfloat16
F32 = jnp.float32


def pieces_dot(ref, weights, width):
    acc = None
    for k in range(ref.shape[0]):
        part = jnp.dot(
            ref[k], weights[k * width : (k + 1) * width, :], preferred_element_type=F32
        )
        acc = part if acc is None else acc + part
    return acc


def hidden_kernel(rows, gate_up, out):
    width = rows.shape[2]
    total = rows.shape[0] * width
    acc = pieces_dot(rows, gate_up, width)
    squares = None
    for k in range(rows.shape[0]):
        values = rows[k].astype(F32)
        part = jnp.sum(values * values, axis=-1, keepdims=True)
        squares = part if squares is None else squares + part
    acc = acc * lax.rsqrt(squares / total + 1e-06)
    half = out.shape[1]
    gate, up = acc[:, :half], acc[:, half:]
    out[...] = (gate / (1.0 + jnp.exp(-gate)) * up).astype(out.dtype)


def out_kernel(rows, down, out):
    out[...] = pieces_dot(rows, down, rows.shape[2]).astype(out.dtype)


def row_call(kernel, name, rows, weights, out_width, steps=4):
    pieces, count, width = rows.shape
    block = count // steps
    return pl.pallas_call(
        kernel,
        name=name,
        grid=(steps,),
        in_specs=[
            pl.BlockSpec((pieces, block, width), lambda i: (0, i, 0)),
            pl.BlockSpec(weights.shape, lambda i: (0, 0)),
        ],
        out_specs=pl.BlockSpec((block, out_width), lambda i: (i, 0)),
        out_shape=jax.ShapeDtypeStruct((count, out_width), BF),
    )(rows, weights)


def after(value, *others):
    return lax.optimization_barrier((value, *others))[0]


def both_groups(array):
    copies = jnp.broadcast_to(array[None], (lax.axis_size("gr"), *array.shape))
    return copies.reshape(-1, *array.shape[1:])


def body(prompt, norm_gain, gate_weight, up_weight, down_weight, routes, route_weight):
    experts, rows, cols = gate_weight.shape
    tok_count, width = prompt.shape
    slots_all = experts * SLOTS
    tp = lax.axis_size("tp")

    expert_ids = jnp.arange(experts, dtype=jnp.int32)[None, :]
    first = routes[:, 0:1] == expert_ids
    second = routes[:, 1:2] == expert_ids
    named = (first | second).astype(BF)
    order = jnp.arange(tok_count, dtype=jnp.int32)
    before = (order[None, :] < order[:, None]).astype(BF)
    earlier = jnp.dot(before, named, preferred_element_type=F32)
    slot_first = jnp.sum(jnp.where(first, earlier, 0.0), axis=1).astype(jnp.int32)
    slot_second = jnp.sum(jnp.where(second, earlier, 0.0), axis=1).astype(jnp.int32)
    target_first = routes[:, 0] * SLOTS + slot_first
    target_second = routes[:, 1] * SLOTS + slot_second
    slot_ids = jnp.arange(slots_all, dtype=jnp.int32)[None, :]
    select_first = (target_first[:, None] == slot_ids).astype(BF)
    select_second = (target_second[:, None] == slot_ids).astype(BF)
    outbound = jnp.einsum(
        "ts,td->sd", select_first + select_second, prompt, preferred_element_type=F32
    ).astype(BF)
    moved = lax.all_to_all(
        outbound.reshape(experts, SLOTS, width), "fs", split_axis=0, concat_axis=0, tiled=True
    )
    arrived = lax.all_gather(moved.reshape(1, slots_all, width), "tp", axis=0, tiled=True)

    gain = norm_gain[None, :, None]
    gate_up = jnp.concatenate(
        [(gate_weight * gain).astype(BF), (up_weight * gain).astype(BF)], axis=2
    )
    gate_up = after(both_groups(gate_up), moved)
    gate_up = lax.all_to_all(gate_up, ("gr", "fs"), split_axis=0, concat_axis=0, tiled=True)
    gate_up = gate_up.reshape(-1, 2 * cols)
    gate_new, up_new = gate_up[None, :, :cols], gate_up[None, :, cols:]

    hidden = row_call(hidden_kernel, "hidden", arrived, gate_up, cols)
    hidden_all = lax.all_gather(hidden[None], "tp", axis=0, tiled=True)

    down = after(both_groups(down_weight.astype(BF)), hidden)
    down = lax.all_to_all(down, ("gr", "fs"), split_axis=0, concat_axis=0, tiled=True)
    down = down.reshape(-1, cols)
    summed = row_call(out_kernel, "expert_out", hidden_all, down, cols)
    returned = lax.all_to_all(
        summed.reshape(experts, SLOTS, width), "fs", split_axis=0, concat_axis=0, tiled=True
    ).reshape(slots_all, width)
    down_new = lax.all_to_all(
        after(down, returned).reshape(tp, -1, cols), "tp", split_axis=0, concat_axis=2, tiled=True
    )

    pick_first = jnp.dot(select_first, returned, preferred_element_type=F32)
    pick_second = jnp.dot(select_second, returned, preferred_element_type=F32)
    mixed = route_weight[:, 0:1] * pick_first + route_weight[:, 1:2] * pick_second
    return (gate_new, up_new, down_new, mixed.astype(BF))


def solution(mesh):
    return jax.shard_map(
        body,
        mesh=mesh,
        in_specs=(
            P(("gr", "fs"), "tp"),
            P(("gr", "fs")),
            P(None, ("gr", "fs"), "tp"),
            P(None, ("gr", "fs"), "tp"),
            P(None, ("gr", "fs"), "tp"),
            P(("gr", "fs"), None),
            P(("gr", "fs"), None),
        ),
        out_specs=(
            P("fs", None, "tp"),
            P("fs", None, "tp"),
            P("fs", "tp", None),
            P(("gr", "fs"), "tp"),
        ),
        check_vma=False,
    )
```

```python
import jax
import jax.numpy as jnp
from jax import lax
from jax.experimental import pallas as pl
from jax.experimental.pallas import tpu as pltpu
from jax.sharding import PartitionSpec as P


SLOTS = 32
BF = jnp.bfloat16
F32 = jnp.float32


def pieces_dot(ref, weights):
    rows = jnp.concatenate([ref[k] for k in range(ref.shape[0])], axis=1)
    return jnp.dot(rows, weights[...], preferred_element_type=F32)


def hidden_kernel(rows, gate_up, out):
    width = rows.shape[2]
    total = rows.shape[0] * width
    acc = pieces_dot(rows, gate_up)
    squares = None
    for k in range(rows.shape[0]):
        values = rows[k].astype(F32)
        part = jnp.sum(values * values, axis=-1, keepdims=True)
        squares = part if squares is None else squares + part
    acc = acc * lax.rsqrt(squares / total + 1e-06)
    half = out.shape[1]
    gate, up = acc[:, :half], acc[:, half:]
    out[...] = (gate / (1.0 + jnp.exp(-gate)) * up).astype(out.dtype)


def out_kernel(rows, down, out):
    out[...] = pieces_dot(rows, down).astype(out.dtype)


def row_call(kernel, rows, weights, out_width, steps=4):
    pieces, count, width = rows.shape
    block = count // steps
    return pl.pallas_call(
        kernel,
        grid=(steps,),
        in_specs=[
            pl.BlockSpec((pieces, block, width), lambda i: (0, i, 0)),
            pl.BlockSpec(weights.shape, lambda i: (0, 0)),
        ],
        out_specs=pl.BlockSpec((block, out_width), lambda i: (i, 0)),
        out_shape=jax.ShapeDtypeStruct((count, out_width), BF),
    )(rows, weights)


def place_kernel(here, *refs):
    pieces, out = refs[:-1], refs[-1]
    for k, piece in enumerate(pieces):

        @pl.when(pl.program_id(0) == k)
        def _(piece=piece):
            out[...] = piece[...]


def exchange_units(array, axis):
    count, here = lax.axis_size(axis), lax.axis_index(axis)
    rows, cols = array.shape[0] // count, array.shape[1]
    pieces = []
    for k in range(count):
        block = lax.dynamic_slice_in_dim(array, (here + k) % count * rows, rows, 0)
        if k:
            block = lax.ppermute(block, axis, [(i, (i + k) % count) for i in range(count)])
        pieces.append(block)
    return pl.pallas_call(
        place_kernel,
        name="place",
        grid_spec=pltpu.PrefetchScalarGridSpec(
            num_scalar_prefetch=1,
            grid=(count,),
            in_specs=[pl.BlockSpec((rows, cols), lambda k, at: (0, 0))] * count,
            out_specs=pl.BlockSpec((rows, cols), lambda k, at: (0, (at[0] - k + count) % count)),
        ),
        out_shape=jax.ShapeDtypeStruct((rows, count * cols), array.dtype),
    )(here.reshape(1).astype(jnp.int32), *pieces)


def after(value, *others):
    return lax.optimization_barrier((value, *others))[0]


def both_groups(array):
    copies = jnp.broadcast_to(array[None], (lax.axis_size("gr"), *array.shape))
    return copies.reshape(-1, *array.shape[1:])


def body(prompt, norm_gain, gate_weight, up_weight, down_weight, routes, route_weight):
    experts, _, cols = gate_weight.shape
    tok_count, width = prompt.shape
    slots_all = experts * SLOTS

    expert_ids = jnp.arange(experts, dtype=jnp.int32)[None, :]
    first = routes[:, 0:1] == expert_ids
    second = routes[:, 1:2] == expert_ids
    named = (first | second).astype(BF)
    order = jnp.arange(tok_count, dtype=jnp.int32)
    before = (order[None, :] < order[:, None]).astype(BF)
    earlier = jnp.dot(before, named, preferred_element_type=F32)
    slot_first = jnp.sum(jnp.where(first, earlier, 0.0), axis=1).astype(jnp.int32)
    slot_second = jnp.sum(jnp.where(second, earlier, 0.0), axis=1).astype(jnp.int32)
    target_first = routes[:, 0] * SLOTS + slot_first
    target_second = routes[:, 1] * SLOTS + slot_second
    slot_ids = jnp.arange(slots_all, dtype=jnp.int32)[None, :]
    select_first = (target_first[:, None] == slot_ids).astype(BF)
    select_second = (target_second[:, None] == slot_ids).astype(BF)
    outbound = jnp.einsum(
        "ts,td->sd", select_first + select_second, prompt, preferred_element_type=F32
    ).astype(BF)
    moved = lax.all_to_all(
        outbound.reshape(experts, SLOTS, width), "fs", split_axis=0, concat_axis=0, tiled=True
    )
    arrived = lax.all_gather(moved.reshape(1, slots_all, width), "tp", axis=0, tiled=True)

    gain = norm_gain[None, :, None]
    gate_up = jnp.concatenate(
        [(gate_weight * gain).astype(BF), (up_weight * gain).astype(BF)], axis=2
    )
    gate_up = after(both_groups(gate_up), moved)
    gate_up = lax.all_to_all(gate_up, ("gr", "fs"), split_axis=0, concat_axis=0, tiled=True)
    gate_up = gate_up.reshape(-1, 2 * cols)
    gate_new, up_new = gate_up[None, :, :cols], gate_up[None, :, cols:]

    hidden = row_call(hidden_kernel, arrived, gate_up, cols)
    hidden_all = lax.all_gather(hidden[None], "tp", axis=0, tiled=True)

    down = after(both_groups(down_weight.astype(BF)), hidden)
    down = lax.all_to_all(down, ("gr", "fs"), split_axis=0, concat_axis=0, tiled=True)
    down = down.reshape(-1, cols)
    summed = row_call(out_kernel, hidden_all, down, cols)
    returned = lax.all_to_all(
        summed.reshape(experts, SLOTS, width), "fs", split_axis=0, concat_axis=0, tiled=True
    )
    returned = returned.reshape(slots_all, width)
    down_new = exchange_units(down, "tp")

    pick_first = jnp.dot(select_first, returned, preferred_element_type=F32)
    pick_second = jnp.dot(select_second, returned, preferred_element_type=F32)
    mixed = route_weight[:, 0:1] * pick_first + route_weight[:, 1:2] * pick_second
    return (gate_new, up_new, down_new[None], mixed.astype(BF))


def solution(mesh):
    return jax.shard_map(
        body,
        mesh=mesh,
        in_specs=(
            P(("gr", "fs"), "tp"),
            P(("gr", "fs")),
            P(None, ("gr", "fs"), "tp"),
            P(None, ("gr", "fs"), "tp"),
            P(None, ("gr", "fs"), "tp"),
            P(("gr", "fs"), None),
            P(("gr", "fs"), None),
        ),
        out_specs=(
            P("fs", None, "tp"),
            P("fs", None, "tp"),
            P("fs", "tp", None),
            P(("gr", "fs"), "tp"),
        ),
        check_vma=False,
    )
```

```python
import jax
import jax.numpy as jnp
from jax import lax
from jax.experimental import pallas as pl
from jax.experimental.pallas import tpu as pltpu
from jax.sharding import PartitionSpec as P


SLOTS = 32
LANES = 128
BF = jnp.bfloat16
F32 = jnp.float32


def pieces_dot(sender, pieces, weights):
    acc = None
    for k, piece in enumerate(pieces):
        at = pl.multiple_of(sender[k] * piece.shape[1], piece.shape[1])
        part = jnp.dot(
            piece[...], weights[pl.ds(at, piece.shape[1]), :], preferred_element_type=F32
        )
        acc = part if acc is None else acc + part
    return acc


def scale_kernel(*refs):
    pieces, out = refs[:-1], refs[-1]
    total = sum(piece.shape[1] for piece in pieces)
    squares = None
    for piece in pieces:
        values = piece[...].astype(F32)
        part = jnp.sum(values * values, axis=-1, keepdims=True)
        squares = part if squares is None else squares + part
    out[...] = jnp.broadcast_to(lax.rsqrt(squares / total + 1e-06), out.shape)


def row_scale(pieces, steps=4):
    count, width = pieces[0].shape
    block = count // steps
    return pl.pallas_call(
        scale_kernel,
        name="row_scale",
        grid=(steps,),
        in_specs=[pl.BlockSpec((block, width), lambda i: (i, 0))] * len(pieces),
        out_specs=pl.BlockSpec((block, LANES), lambda i: (i, 0)),
        out_shape=jax.ShapeDtypeStruct((count, LANES), F32),
        compiler_params=pltpu.CompilerParams(vmem_limit_bytes=8 * 1024 * 1024),
    )(*pieces)


def hidden_kernel(sender, *refs):
    pieces, scale, gate_up, out = refs[:-3], refs[-3], refs[-2], refs[-1]
    half = out.shape[1]
    acc = pieces_dot(sender, pieces, gate_up) * scale[:, :1]
    gate, up = acc[:, :half], acc[:, half:]
    out[...] = (gate / (1.0 + jnp.exp(-gate)) * up).astype(out.dtype)


def out_kernel(sender, *refs):
    out = refs[-1]
    out[...] = pieces_dot(sender, refs[:-2], refs[-2]).astype(out.dtype)


def row_call(kernel, sender, rows, weights, out_width, steps=4):
    count = rows[0].shape[0]
    block = count // steps
    return pl.pallas_call(
        kernel,
        grid_spec=pltpu.PrefetchScalarGridSpec(
            num_scalar_prefetch=1,
            grid=(steps,),
            in_specs=[pl.BlockSpec((block, r.shape[1]), lambda i, at: (i, 0)) for r in rows]
            + [pl.BlockSpec(weights.shape, lambda i, at: (0, 0))],
            out_specs=pl.BlockSpec((block, out_width), lambda i, at: (i, 0)),
        ),
        out_shape=jax.ShapeDtypeStruct((count, out_width), BF),
    )(sender, *rows, weights)


def gather_pieces(piece, axis):
    count = lax.axis_size(axis)

    def shift(value, by):
        return lax.ppermute(value, axis, [(i, (i + by) % count) for i in range(count)])

    def partner(value):
        return lax.ppermute(value, axis, [(i, i ^ 1) for i in range(count)])

    steps = [2, count - 2] + list(range(4, count - 2, 2))
    same = [shift(piece, by) for by in steps]
    own = [piece, *same]
    return own + [partner(value) for value in own]


def piece_senders(axis):
    count, here = lax.axis_size(axis), lax.axis_index(axis)
    steps = jnp.array([0, 2, count - 2] + list(range(4, count - 2, 2)), jnp.int32)
    other = here + 1 - 2 * (here % 2)
    return jnp.concatenate([(here - steps) % count, (other - steps) % count]).astype(jnp.int32)


def place_kernel(here, *refs):
    pieces, out = refs[:-1], refs[-1]
    for k, piece in enumerate(pieces):

        @pl.when(pl.program_id(0) == k)
        def _(piece=piece):
            out[...] = piece[...]


def exchange_units(array, axis):
    count, here = lax.axis_size(axis), lax.axis_index(axis)
    rows, cols = array.shape[0] // count, array.shape[1]
    pieces = []
    for k in range(count):
        block = lax.dynamic_slice_in_dim(array, (here + k) % count * rows, rows, 0)
        if k:
            block = lax.ppermute(block, axis, [(i, (i + k) % count) for i in range(count)])
        pieces.append(block)
    return pl.pallas_call(
        place_kernel,
        name="place",
        grid_spec=pltpu.PrefetchScalarGridSpec(
            num_scalar_prefetch=1,
            grid=(count,),
            in_specs=[pl.BlockSpec((rows, cols), lambda k, at: (0, 0))] * count,
            out_specs=pl.BlockSpec((rows, cols), lambda k, at: (0, (at[0] - k + count) % count)),
        ),
        out_shape=jax.ShapeDtypeStruct((rows, count * cols), array.dtype),
        compiler_params=pltpu.CompilerParams(vmem_limit_bytes=8 * 1024 * 1024),
    )(here.reshape(1).astype(jnp.int32), *pieces)


def after(value, *others):
    return lax.optimization_barrier((value, *others))[0]


def both_groups(array):
    copies = jnp.broadcast_to(array[None], (lax.axis_size("gr"), *array.shape))
    return copies.reshape(-1, *array.shape[1:])


def body(prompt, norm_gain, gate_weight, up_weight, down_weight, routes, route_weight):
    experts, _, cols = gate_weight.shape
    tok_count, width = prompt.shape
    slots_all = experts * SLOTS

    expert_ids = jnp.arange(experts, dtype=jnp.int32)[None, :]
    first = routes[:, 0:1] == expert_ids
    second = routes[:, 1:2] == expert_ids
    named = (first | second).astype(BF)
    order = jnp.arange(tok_count, dtype=jnp.int32)
    before = (order[None, :] < order[:, None]).astype(BF)
    earlier = jnp.dot(before, named, preferred_element_type=F32)
    slot_first = jnp.sum(jnp.where(first, earlier, 0.0), axis=1).astype(jnp.int32)
    slot_second = jnp.sum(jnp.where(second, earlier, 0.0), axis=1).astype(jnp.int32)
    target_first = routes[:, 0] * SLOTS + slot_first
    target_second = routes[:, 1] * SLOTS + slot_second
    slot_ids = jnp.arange(slots_all, dtype=jnp.int32)[None, :]
    select_first = (target_first[:, None] == slot_ids).astype(BF)
    select_second = (target_second[:, None] == slot_ids).astype(BF)
    weighted = jnp.where(
        target_first[:, None] == slot_ids,
        route_weight[:, 0:1],
        jnp.where(target_second[:, None] == slot_ids, route_weight[:, 1:2], 0.0),
    ).astype(BF)
    outbound = jnp.einsum(
        "ts,td->sd", select_first + select_second, prompt, preferred_element_type=F32
    ).astype(BF)
    moved = lax.all_to_all(
        outbound.reshape(experts, SLOTS, width), "fs", split_axis=0, concat_axis=0, tiled=True
    )
    arrived = gather_pieces(moved.reshape(slots_all, width), "tp")
    scale = row_scale(arrived)
    sender = piece_senders("tp")

    gain = norm_gain[None, :, None]
    gate_up = jnp.concatenate(
        [(gate_weight * gain).astype(BF), (up_weight * gain).astype(BF)], axis=2
    )
    gate_up = after(both_groups(gate_up), moved)
    gate_up = lax.all_to_all(gate_up, ("gr", "fs"), split_axis=0, concat_axis=0, tiled=True)
    gate_up = gate_up.reshape(-1, 2 * cols)
    gate_new, up_new = gate_up[None, :, :cols], gate_up[None, :, cols:]

    down = after(both_groups(down_weight.astype(BF)), gate_up)
    down = lax.all_to_all(down, ("gr", "fs"), split_axis=0, concat_axis=0, tiled=True)
    down = down.reshape(-1, cols)

    hidden = row_call(hidden_kernel, sender, [*arrived, scale], gate_up, cols)
    hidden_all = gather_pieces(hidden, "tp")
    summed = row_call(out_kernel, sender, hidden_all, down, cols)
    returned = lax.all_to_all(
        summed.reshape(experts, SLOTS, width), "fs", split_axis=0, concat_axis=0, tiled=True
    )
    returned = returned.reshape(slots_all, width)
    down_new = exchange_units(down, "tp")

    mixed = jnp.dot(weighted, returned, preferred_element_type=F32)
    return (gate_new, up_new, down_new[None], mixed.astype(BF))


def solution(mesh):
    return jax.shard_map(
        body,
        mesh=mesh,
        in_specs=(
            P(("gr", "fs"), "tp"),
            P(("gr", "fs")),
            P(None, ("gr", "fs"), "tp"),
            P(None, ("gr", "fs"), "tp"),
            P(None, ("gr", "fs"), "tp"),
            P(("gr", "fs"), None),
            P(("gr", "fs"), None),
        ),
        out_specs=(
            P("fs", None, "tp"),
            P("fs", None, "tp"),
            P("fs", "tp", None),
            P(("gr", "fs"), "tp"),
        ),
        check_vma=False,
    )
```

```python
import functools

import jax
import jax.numpy as jnp
from jax import lax
from jax.experimental import pallas as pl
from jax.experimental.pallas import tpu as pltpu
from jax.sharding import PartitionSpec as P


SLOTS = 32
LANES = 128
STEPS = 2
BF = jnp.bfloat16
F32 = jnp.float32


def block_of(piece):
    if isinstance(piece, tuple):
        return jnp.where(pl.program_id(0) == 0, piece[0][...], piece[1][...])
    return piece[...]


def paired(refs, layout):
    refs = list(refs)
    return [
        (refs.pop(0), refs.pop(0)) if isinstance(piece, tuple) else refs.pop(0) for piece in layout
    ]


def flat(pieces):
    return [r for piece in pieces for r in (piece if isinstance(piece, tuple) else (piece,))]


def pieces_dot(sender, pieces, weights):
    acc = None
    for k, piece in enumerate(pieces):
        block = block_of(piece)
        at = pl.multiple_of(sender[k] * block.shape[1], block.shape[1])
        part = jnp.dot(block, weights[pl.ds(at, block.shape[1]), :], preferred_element_type=F32)
        acc = part if acc is None else acc + part
    return acc


def scale_kernel(layout, *refs):
    pieces, out = paired(refs[:-1], layout), refs[-1]
    squares, total = None, 0
    for piece in pieces:
        values = block_of(piece).astype(F32)
        total += values.shape[1]
        part = jnp.sum(values * values, axis=-1, keepdims=True)
        squares = part if squares is None else squares + part
    out[...] = jnp.broadcast_to(lax.rsqrt(squares / total + 1e-06), out.shape)


def row_specs(pieces, block):
    return [
        pl.BlockSpec((block, r.shape[1]), lambda i, *_, half=r.shape[0] == block: (0 if half else i, 0))
        for r in flat(pieces)
    ]


def row_scale(pieces):
    count = pieces[0].shape[0]
    return pl.pallas_call(
        functools.partial(scale_kernel, pieces),
        name="row_scale",
        grid=(STEPS,),
        in_specs=row_specs(pieces, count // STEPS),
        out_specs=pl.BlockSpec((count // STEPS, LANES), lambda i: (i, 0)),
        out_shape=jax.ShapeDtypeStruct((count, LANES), F32),
        compiler_params=pltpu.CompilerParams(vmem_limit_bytes=12 * 1024 * 1024),
    )(*flat(pieces))


def hidden_kernel(layout, sender, *refs):
    scale, gate_up, out = refs[-3:]
    half = out.shape[1]
    acc = pieces_dot(sender, paired(refs[:-3], layout), gate_up) * scale[:, :1]
    gate, up = acc[:, :half], acc[:, half:]
    out[...] = (gate / (1.0 + jnp.exp(-gate)) * up).astype(out.dtype)


def out_kernel(layout, sender, *refs):
    down, out = refs[-2:]
    out[...] = pieces_dot(sender, paired(refs[:-2], layout), down).astype(out.dtype)


def row_call(kernel, sender, pieces, others, weights, out_width):
    count = pieces[0].shape[0]
    block = count // STEPS
    return pl.pallas_call(
        functools.partial(kernel, pieces),
        grid_spec=pltpu.PrefetchScalarGridSpec(
            num_scalar_prefetch=1,
            grid=(STEPS,),
            in_specs=row_specs([*pieces, *others], block)
            + [pl.BlockSpec(weights.shape, lambda i, at: (0, 0))],
            out_specs=pl.BlockSpec((block, out_width), lambda i, at: (i, 0)),
        ),
        out_shape=jax.ShapeDtypeStruct((count, out_width), BF),
    )(sender, *flat(pieces), *others, weights)


def shift(value, axis, by):
    count = lax.axis_size(axis)
    return lax.ppermute(value, axis, [(i, (i + by) % count) for i in range(count)])


def partner(value, axis):
    return lax.ppermute(value, axis, [(i, i ^ 1) for i in range(lax.axis_size(axis))])


def gather_pieces(piece, axis):
    half = piece.shape[0] // 2
    right, left = shift(piece, axis, 2), shift(piece, axis, -2)
    other = partner(piece, axis)
    far = (shift(right[:half], axis, 2), shift(left[half:], axis, -2))
    return [
        piece,
        right,
        left,
        far,
        other,
        partner(right, axis),
        partner(left, axis),
        tuple(partner(value, axis) for value in far),
    ]


def piece_senders(axis):
    count, here = lax.axis_size(axis), lax.axis_index(axis)
    other = here + 1 - 2 * (here % 2)
    return jnp.stack([(at - by) % count for at in (here, other) for by in (0, 2, -2, 4)]).astype(
        jnp.int32
    )


def place_kernel(at, *refs):
    pieces, out = refs[:-1], refs[-1]
    for k, piece in enumerate(pieces):

        @pl.when(pl.program_id(0) // 2 == k)
        def _(piece=piece):
            out[...] = piece[pl.program_id(0) % 2]


def exchange_units(array, axis):
    count, here = lax.axis_size(axis), lax.axis_index(axis)
    chips, chip, core = count // 2, here // 2, here % 2
    rows, cols = array.shape[0] // count, array.shape[1]
    blocks = array.reshape(chips, 2, rows, cols)
    mine = lax.dynamic_slice_in_dim(blocks, core, 1, 1)
    theirs = partner(lax.dynamic_slice_in_dim(blocks, 1 - core, 1, 1), axis)
    both = jnp.concatenate([mine, theirs], axis=1)
    pieces = []
    for k in range(chips):
        block = lax.dynamic_slice_in_dim(both, (chip + k) % chips, 1, 0)[0]
        pieces.append(shift(block, axis, 2 * k) if k else block)
    places = [
        2 * ((chip - k) % chips) + side for k in range(chips) for side in (core, 1 - core)
    ]
    return pl.pallas_call(
        place_kernel,
        name="place",
        grid_spec=pltpu.PrefetchScalarGridSpec(
            num_scalar_prefetch=1,
            grid=(count,),
            in_specs=[pl.BlockSpec((2, rows, cols), lambda k, at: (0, 0, 0))] * chips,
            out_specs=pl.BlockSpec((rows, cols), lambda k, at: (0, at[k])),
        ),
        out_shape=jax.ShapeDtypeStruct((rows, count * cols), array.dtype),
        compiler_params=pltpu.CompilerParams(vmem_limit_bytes=8 * 1024 * 1024),
    )(jnp.stack(places).astype(jnp.int32), *pieces)


def after(value, *others):
    return lax.optimization_barrier((value, *others))[0]


def both_groups(array):
    copies = jnp.broadcast_to(array[None], (lax.axis_size("gr"), *array.shape))
    return copies.reshape(-1, *array.shape[1:])


def body(prompt, norm_gain, gate_weight, up_weight, down_weight, routes, route_weight):
    experts, _, cols = gate_weight.shape
    tok_count, width = prompt.shape
    slots_all = experts * SLOTS

    expert_ids = jnp.arange(experts, dtype=jnp.int32)[None, :]
    first = routes[:, 0:1] == expert_ids
    second = routes[:, 1:2] == expert_ids
    named = (first | second).astype(BF)
    order = jnp.arange(tok_count, dtype=jnp.int32)
    before = (order[None, :] < order[:, None]).astype(BF)
    earlier = jnp.dot(before, named, preferred_element_type=F32)
    slot_first = jnp.sum(jnp.where(first, earlier, 0.0), axis=1).astype(jnp.int32)
    slot_second = jnp.sum(jnp.where(second, earlier, 0.0), axis=1).astype(jnp.int32)
    target_first = routes[:, 0] * SLOTS + slot_first
    target_second = routes[:, 1] * SLOTS + slot_second
    slot_ids = jnp.arange(slots_all, dtype=jnp.int32)[None, :]
    select_first = (target_first[:, None] == slot_ids).astype(BF)
    select_second = (target_second[:, None] == slot_ids).astype(BF)
    weighted = jnp.where(
        target_first[:, None] == slot_ids,
        route_weight[:, 0:1],
        jnp.where(target_second[:, None] == slot_ids, route_weight[:, 1:2], 0.0),
    ).astype(BF)
    outbound = jnp.einsum(
        "ts,td->sd", select_first + select_second, prompt, preferred_element_type=F32
    ).astype(BF)
    moved = lax.all_to_all(
        outbound.reshape(experts, SLOTS, width), "fs", split_axis=0, concat_axis=0, tiled=True
    )
    arrived = gather_pieces(moved.reshape(slots_all, width), "tp")
    scale = row_scale(arrived)
    sender = piece_senders("tp")

    gain = norm_gain[None, :, None]
    gate_up = jnp.concatenate(
        [(gate_weight * gain).astype(BF), (up_weight * gain).astype(BF)], axis=2
    )
    gate_up = both_groups(gate_up)
    gate_up = after(gate_up, moved)
    gate_up = lax.all_to_all(gate_up, ("gr", "fs"), split_axis=0, concat_axis=0, tiled=True)
    gate_up = gate_up.reshape(-1, 2 * cols)
    gate_new, up_new = gate_up[None, :, :cols], gate_up[None, :, cols:]

    down = both_groups(down_weight.astype(BF))
    down = after(down, gate_up)
    down = lax.all_to_all(down, ("gr", "fs"), split_axis=0, concat_axis=0, tiled=True)
    down = down.reshape(-1, cols)

    hidden = row_call(hidden_kernel, sender, arrived, [scale], gate_up, cols)
    hidden_all = gather_pieces(hidden, "tp")
    summed = row_call(out_kernel, sender, hidden_all, [], down, cols)
    returned = lax.all_to_all(
        summed.reshape(experts, SLOTS, width), "fs", split_axis=0, concat_axis=0, tiled=True
    )
    returned = returned.reshape(slots_all, width)
    down_new = exchange_units(down, "tp")

    mixed = jnp.dot(weighted, returned, preferred_element_type=F32)
    return (gate_new, up_new, down_new[None], mixed.astype(BF))


def solution(mesh):
    return jax.shard_map(
        body,
        mesh=mesh,
        in_specs=(
            P(("gr", "fs"), "tp"),
            P(("gr", "fs")),
            P(None, ("gr", "fs"), "tp"),
            P(None, ("gr", "fs"), "tp"),
            P(None, ("gr", "fs"), "tp"),
            P(("gr", "fs"), None),
            P(("gr", "fs"), None),
        ),
        out_specs=(
            P("fs", None, "tp"),
            P("fs", None, "tp"),
            P("fs", "tp", None),
            P(("gr", "fs"), "tp"),
        ),
        check_vma=False,
    )
```

```python
import jax
import jax.numpy as jnp
from jax import lax
from jax.experimental import pallas as pl
from jax.experimental.pallas import tpu as pltpu
from jax.sharding import Mesh
from jax.sharding import PartitionSpec as P


SLOTS = 32
HALF = SLOTS // 2
LANES = 128
BF = jnp.bfloat16
F32 = jnp.float32
ANY = pl.BlockSpec(memory_space=pl.ANY)
WHOLE = pl.BlockSpec(memory_space=pltpu.VMEM)
SCALARS = pl.BlockSpec(memory_space=pltpu.SMEM)


def scale_kernel(*refs):
    pieces, out = refs[:-1], refs[-1]
    squares, total = None, 0
    for piece in pieces:
        for j in range(2):
            values = piece[j].astype(F32)
            total += values.shape[1]
            part = jnp.sum(values * values, axis=-1, keepdims=True)
            squares = part if squares is None else squares + part
    out[...] = jnp.broadcast_to(lax.rsqrt(squares / total + 1e-06), out.shape)


def row_scale(pieces):
    count = pieces[0].shape[1]
    return pl.pallas_call(
        scale_kernel,
        name="row_scale",
        in_specs=[WHOLE] * len(pieces),
        out_specs=WHOLE,
        out_shape=jax.ShapeDtypeStruct((count, LANES), F32),
        compiler_params=pltpu.CompilerParams(vmem_limit_bytes=12 * 1024 * 1024),
    )(*pieces)


def fetch(source, target, sem):
    copy = pltpu.make_async_copy(source, target, sem)
    copy.start()
    return copy


def joined(rows, k):
    return jnp.concatenate([rows[k, 0], rows[k, 1]], axis=1)


def hidden_kernel(chip, *refs):
    pieces, (scale, mine, theirs, out, rows, weights, row_sems, weight_sems) = refs[:-8], refs[-8:]
    chips = len(pieces)
    width = 2 * rows.shape[3]
    row_copies, weight_copies = [], {}
    for j, source in enumerate((mine, theirs)):
        for k in range(chips):
            if j == 0:
                row_copies.append(fetch(pieces[k], rows.at[k], row_sems.at[k]))
            at = pl.multiple_of(chip[k] * width, width)
            weight_copies[j, k] = fetch(
                source.at[pl.ds(at, width)], weights.at[j, k], weight_sems.at[j, k]
            )
    half = out.shape[2]
    for j in range(2):
        acc = None
        for k in range(chips):
            if j == 0:
                row_copies[k].wait()
            weight_copies[j, k].wait()
            part = jnp.dot(joined(rows, k), weights[j, k], preferred_element_type=F32)
            acc = part if acc is None else acc + part
        acc = acc * scale[:, :1]
        gate, up = acc[:, :half], acc[:, half:]
        out[j] = (gate / (1.0 + jnp.exp(-gate)) * up).astype(out.dtype)


def hidden_call(chip, pieces, scale, mine, theirs):
    sides, count, width = pieces[0].shape
    chips = len(pieces)
    return pl.pallas_call(
        hidden_kernel,
        name="hidden",
        in_specs=[SCALARS] + [ANY] * chips + [WHOLE, ANY, ANY],
        out_specs=WHOLE,
        out_shape=jax.ShapeDtypeStruct((2, count, mine.shape[1] // 2), BF),
        scratch_shapes=[
            pltpu.VMEM((chips, sides, count, width), BF),
            pltpu.VMEM((2, chips, sides * width, mine.shape[1]), BF),
            pltpu.SemaphoreType.DMA((chips,)),
            pltpu.SemaphoreType.DMA((2, chips)),
        ],
    )(chip, *pieces, scale, mine, theirs)


def out_kernel(block, leaving, core, *refs):
    chips = leaving.shape[0]
    pieces, mine, theirs, out = refs[:chips], *refs[chips : chips + 3]
    blocks = refs[chips + 3 : 2 * chips + 3]
    rows, weights, row_sems, weight_sems, block_sems = refs[2 * chips + 3 :]
    width = rows.shape[3]
    cols = out.shape[2]
    row_copies, weight_copies = [], {}
    for k in range(chips):
        row_copies.append(fetch(pieces[k], rows.at[k], row_sems.at[k]))
        for side in range(2):
            at = pl.multiple_of(block[2 * k + side] * width, width)
            for j, source in enumerate((mine, theirs)):
                weight_copies[k, side, j] = fetch(
                    source.at[pl.ds(at, width)],
                    weights.at[k, pl.ds(side * width, width), pl.ds(j * cols, cols)],
                    weight_sems.at[k, side, j],
                )
    block_copies = []
    for k in range(chips):
        at = pl.multiple_of(leaving[k] * width, width)
        for j, source in enumerate((mine, theirs)):
            block_copies.append(
                fetch(source.at[pl.ds(at, width)], blocks[k].at[j], block_sems.at[k, j])
            )
    acc = None
    for k in range(chips):
        row_copies[k].wait()
        for side in range(2):
            for j in range(2):
                weight_copies[k, side, j].wait()
        part = jnp.dot(joined(rows, k), weights[k], preferred_element_type=F32)
        acc = part if acc is None else acc + part
    out[core[0]] = acc[:, :cols].astype(out.dtype)
    out[1 - core[0]] = acc[:, cols:].astype(out.dtype)
    for copy in block_copies:
        copy.wait()


def out_call(block, leaving, core, pieces, mine, theirs):
    sides, count, width = pieces[0].shape
    chips, cols = len(pieces), mine.shape[1]
    return pl.pallas_call(
        out_kernel,
        name="expert_out",
        in_specs=[SCALARS] * 3 + [ANY] * (chips + 2),
        out_specs=[WHOLE] + [ANY] * chips,
        out_shape=[jax.ShapeDtypeStruct((2, count, cols), BF)]
        + [jax.ShapeDtypeStruct((2, width, cols), BF)] * chips,
        scratch_shapes=[
            pltpu.VMEM((chips, sides, count, width), BF),
            pltpu.VMEM((chips, sides * width, 2 * cols), BF),
            pltpu.SemaphoreType.DMA((chips,)),
            pltpu.SemaphoreType.DMA((chips, 2, 2)),
            pltpu.SemaphoreType.DMA((chips, 2)),
        ],
    )(block, leaving, core, *pieces, mine, theirs)


def place_kernel(chip, core, *refs):
    pieces, out = refs[:-1], refs[-1]
    for k, piece in enumerate(pieces):

        @pl.when(pl.program_id(0) == k)
        def _(piece=piece):
            out[...] = jnp.concatenate([piece[core[0]], piece[1 - core[0]]], axis=1)


def place_call(chip, core, pieces):
    sides, rows, cols = pieces[0].shape
    chips = len(pieces)
    return pl.pallas_call(
        place_kernel,
        name="place",
        grid_spec=pltpu.PrefetchScalarGridSpec(
            num_scalar_prefetch=2,
            grid=(chips,),
            in_specs=[pl.BlockSpec((sides, rows, cols), lambda k, *_: (0, 0, 0))] * chips,
            out_specs=pl.BlockSpec((rows, sides * cols), lambda k, chip, core: (0, chip[k])),
        ),
        out_shape=jax.ShapeDtypeStruct((rows, chips * sides * cols), BF),
        compiler_params=pltpu.CompilerParams(vmem_limit_bytes=8 * 1024 * 1024),
    )(chip, core, *pieces)


def shift(value, by):
    count = lax.axis_size("x")
    return lax.ppermute(value, "x", [(i, (i + by) % count) for i in range(count)])


def swap(value):
    return lax.ppermute(value, "c", [(0, 1), (1, 0)])


def spread(value, offsets):
    return [shift(value, by) if by else value for by in offsets]


def spread_each(values):
    return [shift(value, by) if by else value for by, value in enumerate(values)]


def exchange(value, axes):
    return lax.all_to_all(value, axes, split_axis=0, concat_axis=0, tiled=True)


def after(value, *others):
    return lax.optimization_barrier((value, *others))[0]


def both_groups(array):
    copies = jnp.broadcast_to(array[None], (lax.axis_size("gr"), *array.shape))
    return copies.reshape(-1, *array.shape[1:])


def body(prompt, norm_gain, gate_weight, up_weight, down_weight, routes, route_weight):
    experts, _, cols = gate_weight.shape
    tok_count, width = prompt.shape
    slots_all = experts * SLOTS
    half_all = slots_all // 2
    chips = lax.axis_size("x")
    chip, core = lax.axis_index("x"), lax.axis_index("c")
    offsets = [0, 1, chips - 1] + list(range(2, chips - 1))
    senders = [(chip - by) % chips for by in offsets]
    sender = jnp.stack(senders).astype(jnp.int32)
    units = jnp.stack([2 * at + side for at in senders for side in (core, 1 - core)])
    units = units.astype(jnp.int32)
    core_id = core.reshape(1).astype(jnp.int32)

    expert_ids = jnp.arange(experts, dtype=jnp.int32)[None, :]
    first = routes[:, 0:1] == expert_ids
    second = routes[:, 1:2] == expert_ids
    named = (first | second).astype(BF)
    order = jnp.arange(tok_count, dtype=jnp.int32)
    before = (order[None, :] < order[:, None]).astype(BF)
    earlier = jnp.dot(before, named, preferred_element_type=F32)
    slot_first = jnp.sum(jnp.where(first, earlier, 0.0), axis=1).astype(jnp.int32)
    slot_second = jnp.sum(jnp.where(second, earlier, 0.0), axis=1).astype(jnp.int32)

    def row_of(expert, slot):
        return slot // HALF * half_all + expert * HALF + slot % HALF

    target_first = row_of(routes[:, 0], slot_first)
    target_second = row_of(routes[:, 1], slot_second)
    slot_ids = jnp.arange(slots_all, dtype=jnp.int32)[None, :]
    is_first = target_first[:, None] == slot_ids
    is_second = target_second[:, None] == slot_ids
    weighted = jnp.where(
        is_first, route_weight[:, 0:1], jnp.where(is_second, route_weight[:, 1:2], 0.0)
    ).astype(BF)
    outbound = jnp.einsum(
        "ts,td->sd", (is_first | is_second).astype(BF), prompt, preferred_element_type=F32
    ).astype(BF)
    moved = exchange(outbound.reshape(2 * experts, HALF, width), ("c", "fs"))
    arrived = spread(moved.reshape(2, half_all, width), offsets)
    scale = row_scale(arrived)

    gain = norm_gain[None, :, None]
    gate_up = jnp.concatenate(
        [(gate_weight * gain).astype(BF), (up_weight * gain).astype(BF)], axis=2
    )
    gate_up = both_groups(gate_up)
    gate_up = after(gate_up, moved)
    gate_up = exchange(gate_up, ("gr", "fs"))
    gate_up = gate_up.reshape(-1, 2 * cols)
    gate_up_other = swap(gate_up)
    gate_new, up_new = gate_up[None, :, :cols], gate_up[None, :, cols:]

    down = both_groups(down_weight.astype(BF))
    down = after(down, gate_up)
    down = exchange(down, ("gr", "fs"))
    down = down.reshape(-1, cols)
    down_other = swap(down)

    hidden = hidden_call(sender, arrived, scale, gate_up, gate_up_other)
    hidden_all = spread(hidden, offsets)
    leaving = jnp.stack([2 * ((chip + by) % chips) + core for by in range(chips)])
    summed, *blocks = out_call(
        units, leaving.astype(jnp.int32), core_id, hidden_all, down, down_other
    )

    returned = exchange(summed.reshape(2 * experts, HALF, width), ("c", "fs"))
    returned = returned.reshape(slots_all, width)
    pieces = spread_each(blocks)
    places = jnp.stack([(chip - by) % chips for by in range(chips)]).astype(jnp.int32)
    down_new = place_call(places, core_id, pieces)

    mixed = jnp.dot(weighted, returned, preferred_element_type=F32)
    return (gate_new, up_new, down_new[None], mixed.astype(BF))


def solution(mesh):
    groups, servers, shards = mesh.devices.shape
    devices = mesh.devices.reshape(groups, servers, shards // 2, 2)
    tp = ("x", "c")
    return jax.shard_map(
        body,
        mesh=Mesh(devices, ("gr", "fs", "x", "c")),
        in_specs=(
            P(("gr", "fs"), tp),
            P(("gr", "fs")),
            P(None, ("gr", "fs"), tp),
            P(None, ("gr", "fs"), tp),
            P(None, ("gr", "fs"), tp),
            P(("gr", "fs"), None),
            P(("gr", "fs"), None),
        ),
        out_specs=(
            P("fs", None, tp),
            P("fs", None, tp),
            P("fs", tp, None),
            P(("gr", "fs"), tp),
        ),
        check_vma=False,
    )
```

```python
import jax
import jax.numpy as jnp
from jax import lax
from jax.experimental import pallas as pl
from jax.experimental.pallas import tpu as pltpu
from jax.sharding import Mesh
from jax.sharding import PartitionSpec as P


SLOTS = 32
HALF = SLOTS // 2
LANES = 128
BF = jnp.bfloat16
F32 = jnp.float32
ANY = pl.BlockSpec(memory_space=pl.ANY)
WHOLE = pl.BlockSpec(memory_space=pltpu.VMEM)
SCALARS = pl.BlockSpec(memory_space=pltpu.SMEM)


def scale_kernel(*refs):
    pieces, out = refs[:-1], refs[-1]
    squares, total = None, 0
    for piece in pieces:
        for j in range(2):
            values = piece[j].astype(F32)
            total += values.shape[1]
            part = jnp.sum(values * values, axis=-1, keepdims=True)
            squares = part if squares is None else squares + part
    out[...] = jnp.broadcast_to(lax.rsqrt(squares / total + 1e-06), out.shape)


def row_scale(pieces):
    count = pieces[0].shape[1]
    return pl.pallas_call(
        scale_kernel,
        name="row_scale",
        in_specs=[WHOLE] * len(pieces),
        out_specs=WHOLE,
        out_shape=jax.ShapeDtypeStruct((count, LANES), F32),
        compiler_params=pltpu.CompilerParams(vmem_limit_bytes=12 * 1024 * 1024),
    )(*pieces)


def fetch(source, target, sem):
    copy = pltpu.make_async_copy(source, target, sem)
    copy.start()
    return copy


def joined(rows, k):
    return jnp.concatenate([rows[k, 0], rows[k, 1]], axis=1)


def hidden_kernel(block, *refs):
    pieces, (scale, mine, theirs, out, rows, weights, row_sems, weight_sems) = refs[:-8], refs[-8:]
    chips = len(pieces)
    width = rows.shape[3]
    row_copies, weight_copies = [], {}
    for j, source in enumerate((mine, theirs)):
        for k in range(chips):
            if j == 0:
                row_copies.append(fetch(pieces[k], rows.at[k], row_sems.at[k]))
            for side in range(2):
                at = pl.multiple_of(block[2 * k + side] * width, width)
                weight_copies[j, k, side] = fetch(
                    source.at[pl.ds(at, width)],
                    weights.at[j, k, pl.ds(side * width, width)],
                    weight_sems.at[j, k, side],
                )
    half = out.shape[2]
    for j in range(2):
        acc = None
        for k in range(chips):
            if j == 0:
                row_copies[k].wait()
            for side in range(2):
                weight_copies[j, k, side].wait()
            part = jnp.dot(joined(rows, k), weights[j, k], preferred_element_type=F32)
            acc = part if acc is None else acc + part
        acc = acc * scale[:, :1]
        gate, up = acc[:, :half], acc[:, half:]
        out[j] = (gate / (1.0 + jnp.exp(-gate)) * up).astype(out.dtype)


def hidden_call(block, pieces, scale, mine, theirs):
    sides, count, width = pieces[0].shape
    chips = len(pieces)
    return pl.pallas_call(
        hidden_kernel,
        name="hidden",
        in_specs=[SCALARS] + [ANY] * chips + [WHOLE, ANY, ANY],
        out_specs=WHOLE,
        out_shape=jax.ShapeDtypeStruct((2, count, mine.shape[1] // 2), BF),
        scratch_shapes=[
            pltpu.VMEM((chips, sides, count, width), BF),
            pltpu.VMEM((2, chips, sides * width, mine.shape[1]), BF),
            pltpu.SemaphoreType.DMA((chips,)),
            pltpu.SemaphoreType.DMA((2, chips, 2)),
        ],
    )(block, *pieces, scale, mine, theirs)


def out_kernel(block, core, *refs):
    pieces, (mine, theirs, out, rows, weights, row_sems, weight_sems) = refs[:-7], refs[-7:]
    chips = len(pieces)
    width = rows.shape[3]
    cols = out.shape[2]
    row_copies, weight_copies = [], {}
    for k in range(chips):
        row_copies.append(fetch(pieces[k], rows.at[k], row_sems.at[k]))
        for side in range(2):
            at = pl.multiple_of(block[2 * k + side] * width, width)
            for j, source in enumerate((mine, theirs)):
                weight_copies[k, side, j] = fetch(
                    source.at[pl.ds(at, width)],
                    weights.at[k, pl.ds(side * width, width), pl.ds(j * cols, cols)],
                    weight_sems.at[k, side, j],
                )
    acc = None
    for k in range(chips):
        row_copies[k].wait()
        for side in range(2):
            for j in range(2):
                weight_copies[k, side, j].wait()
        part = jnp.dot(joined(rows, k), weights[k], preferred_element_type=F32)
        acc = part if acc is None else acc + part
    out[core[0]] = acc[:, :cols].astype(out.dtype)
    out[1 - core[0]] = acc[:, cols:].astype(out.dtype)


def out_call(block, core, pieces, mine, theirs):
    sides, count, width = pieces[0].shape
    chips, cols = len(pieces), mine.shape[1]
    return pl.pallas_call(
        out_kernel,
        name="expert_out",
        in_specs=[SCALARS, SCALARS] + [ANY] * (chips + 2),
        out_specs=WHOLE,
        out_shape=jax.ShapeDtypeStruct((2, count, cols), BF),
        scratch_shapes=[
            pltpu.VMEM((chips, sides, count, width), BF),
            pltpu.VMEM((chips, sides * width, 2 * cols), BF),
            pltpu.SemaphoreType.DMA((chips,)),
            pltpu.SemaphoreType.DMA((chips, 2, 2)),
        ],
        compiler_params=pltpu.CompilerParams(vmem_limit_bytes=20 * 1024 * 1024),
    )(block, core, *pieces, mine, theirs)


def cut_kernel(leaving, mine, theirs, *outs):
    width = outs[0].shape[1]
    for k, out in enumerate(outs):
        at = pl.multiple_of(leaving[k] * width, width)
        out[0] = mine[pl.ds(at, width), :]
        out[1] = theirs[pl.ds(at, width), :]


def cut_call(leaving, mine, theirs, width):
    count = leaving.shape[0]
    return pl.pallas_call(
        cut_kernel,
        name="cut",
        in_specs=[SCALARS, WHOLE, WHOLE],
        out_specs=[WHOLE] * count,
        out_shape=[jax.ShapeDtypeStruct((2, width, mine.shape[1]), BF)] * count,
        compiler_params=pltpu.CompilerParams(vmem_limit_bytes=12 * 1024 * 1024),
    )(leaving, mine, theirs)


def place_kernel(chip, core, *refs):
    pieces, out = refs[:-1], refs[-1]
    for k, piece in enumerate(pieces):

        @pl.when(pl.program_id(0) == k)
        def _(piece=piece):
            out[...] = jnp.concatenate([piece[core[0]], piece[1 - core[0]]], axis=1)


def place_call(chip, core, pieces):
    sides, rows, cols = pieces[0].shape
    chips = len(pieces)
    return pl.pallas_call(
        place_kernel,
        name="place",
        grid_spec=pltpu.PrefetchScalarGridSpec(
            num_scalar_prefetch=2,
            grid=(chips,),
            in_specs=[pl.BlockSpec((sides, rows, cols), lambda k, *_: (0, 0, 0))] * chips,
            out_specs=pl.BlockSpec((rows, sides * cols), lambda k, chip, core: (0, chip[k])),
        ),
        out_shape=jax.ShapeDtypeStruct((rows, chips * sides * cols), BF),
        compiler_params=pltpu.CompilerParams(vmem_limit_bytes=8 * 1024 * 1024),
    )(chip, core, *pieces)


def shift(value, by):
    count = lax.axis_size("x")
    return lax.ppermute(value, "x", [(i, (i + by) % count) for i in range(count)])


def swap(value):
    return lax.ppermute(value, "c", [(0, 1), (1, 0)])


def spread(value, offsets):
    return [shift(value, by) if by else value for by in offsets]


def exchange(value, axes):
    return lax.all_to_all(value, axes, split_axis=0, concat_axis=0, tiled=True)


def after(value, *others):
    return lax.optimization_barrier((value, *others))[0]


def both_groups(array):
    copies = jnp.broadcast_to(array[None], (lax.axis_size("gr"), *array.shape))
    return copies.reshape(-1, *array.shape[1:])


def body(prompt, norm_gain, gate_weight, up_weight, down_weight, routes, route_weight):
    experts, _, cols = gate_weight.shape
    tok_count, width = prompt.shape
    slots_all = experts * SLOTS
    half_all = slots_all // 2
    chips = lax.axis_size("x")
    chip, core = lax.axis_index("x"), lax.axis_index("c")
    offsets = [0, 1, chips - 1] + list(range(2, chips - 1))
    senders = [(chip - by) % chips for by in offsets]
    units = jnp.stack([2 * at + side for at in senders for side in (core, 1 - core)])
    units = units.astype(jnp.int32)
    core_id = core.reshape(1).astype(jnp.int32)

    expert_ids = jnp.arange(experts, dtype=jnp.int32)[None, :]
    first = routes[:, 0:1] == expert_ids
    second = routes[:, 1:2] == expert_ids
    named = (first | second).astype(BF)
    order = jnp.arange(tok_count, dtype=jnp.int32)
    before = (order[None, :] < order[:, None]).astype(BF)
    earlier = jnp.dot(before, named, preferred_element_type=F32)
    slot_first = jnp.sum(jnp.where(first, earlier, 0.0), axis=1).astype(jnp.int32)
    slot_second = jnp.sum(jnp.where(second, earlier, 0.0), axis=1).astype(jnp.int32)

    slot_ids = jnp.arange(slots_all, dtype=jnp.int32)[None, :]

    def picks(place):
        at_first = place(routes[:, 0], slot_first)[:, None] == slot_ids
        return at_first, place(routes[:, 1], slot_second)[:, None] == slot_ids

    is_first, is_second = picks(lambda expert, slot: expert * SLOTS + slot)
    outbound = jnp.einsum(
        "ts,td->sd", (is_first | is_second).astype(BF), prompt, preferred_element_type=F32
    ).astype(BF)
    moved = exchange(outbound.reshape(experts, SLOTS, width), "fs")
    halves = moved.reshape(experts, 2, HALF, width)
    mine, theirs = (
        lax.dynamic_slice_in_dim(halves, at, 1, 1).reshape(half_all, width)
        for at in (core, 1 - core)
    )
    arrived = spread(jnp.stack([mine, swap(theirs)]), offsets)
    is_first, is_second = picks(
        lambda expert, slot: slot // HALF * half_all + expert * HALF + slot % HALF
    )
    weighted = jnp.where(
        is_first, route_weight[:, 0:1], jnp.where(is_second, route_weight[:, 1:2], 0.0)
    ).astype(BF)
    scale = row_scale(arrived)

    gain = norm_gain[None, :, None]
    gate_up = jnp.concatenate(
        [(gate_weight * gain).astype(BF), (up_weight * gain).astype(BF)], axis=2
    )
    gate_up = both_groups(gate_up)
    gate_up = after(gate_up, moved)
    gate_up = exchange(gate_up, ("gr", "fs"))
    gate_up = gate_up.reshape(-1, 2 * cols)
    gate_up_other = swap(gate_up)
    gate_new, up_new = gate_up[None, :, :cols], gate_up[None, :, cols:]

    down = both_groups(down_weight.astype(BF))
    down = after(down, gate_up)
    down = exchange(down, ("gr", "fs"))
    down = down.reshape(-1, cols)
    down_other = swap(down)

    hidden = hidden_call(units, arrived, scale, gate_up, gate_up_other)
    hidden_all = spread(hidden, offsets)
    leaving = jnp.stack([2 * ((chip + by) % chips) + core for by in range(chips)])
    blocks = list(cut_call(leaving.astype(jnp.int32), down, down_other, cols))
    far = chips // 2
    blocks[far] = shift(blocks[far], far)
    summed = out_call(units, core_id, hidden_all, down, down_other)

    returned = exchange(summed.reshape(2 * experts, HALF, width), ("c", "fs"))
    returned = returned.reshape(slots_all, width)
    pieces = [shift(value, by) if by not in (0, far) else value for by, value in enumerate(blocks)]
    places = jnp.stack([(chip - by) % chips for by in range(chips)]).astype(jnp.int32)
    down_new = place_call(places, core_id, pieces)

    mixed = jnp.dot(weighted, returned, preferred_element_type=F32)
    return (gate_new, up_new, down_new[None], mixed.astype(BF))


def solution(mesh):
    groups, servers, shards = mesh.devices.shape
    devices = mesh.devices.reshape(groups, servers, shards // 2, 2)
    tp = ("x", "c")
    return jax.shard_map(
        body,
        mesh=Mesh(devices, ("gr", "fs", "x", "c")),
        in_specs=(
            P(("gr", "fs"), tp),
            P(("gr", "fs")),
            P(None, ("gr", "fs"), tp),
            P(None, ("gr", "fs"), tp),
            P(None, ("gr", "fs"), tp),
            P(("gr", "fs"), None),
            P(("gr", "fs"), None),
        ),
        out_specs=(
            P("fs", None, tp),
            P("fs", None, tp),
            P("fs", tp, None),
            P(("gr", "fs"), tp),
        ),
        check_vma=False,
    )
```

```python
import jax
import jax.numpy as jnp
from jax import lax
from jax.experimental import pallas as pl
from jax.experimental.pallas import tpu as pltpu
from jax.sharding import Mesh
from jax.sharding import PartitionSpec as P


SLOTS = 32
HALF = SLOTS // 2
LANES = 128
BF = jnp.bfloat16
F32 = jnp.float32
ANY = pl.BlockSpec(memory_space=pl.ANY)
WHOLE = pl.BlockSpec(memory_space=pltpu.VMEM)
SCALARS = pl.BlockSpec(memory_space=pltpu.SMEM)


def scale_kernel(*refs):
    pieces, out = refs[:-1], refs[-1]
    squares, total = None, 0
    for piece in pieces:
        for j in range(2):
            values = piece[j].astype(F32)
            total += values.shape[1]
            part = jnp.sum(values * values, axis=-1, keepdims=True)
            squares = part if squares is None else squares + part
    out[...] = jnp.broadcast_to(lax.rsqrt(squares / total + 1e-06), out.shape)


def row_scale(pieces):
    count = pieces[0].shape[1]
    return pl.pallas_call(
        scale_kernel,
        name="row_scale",
        in_specs=[WHOLE] * len(pieces),
        out_specs=WHOLE,
        out_shape=jax.ShapeDtypeStruct((count, LANES), F32),
        compiler_params=pltpu.CompilerParams(vmem_limit_bytes=12 * 1024 * 1024),
    )(*pieces)


def fetch(source, target, sem):
    copy = pltpu.make_async_copy(source, target, sem)
    copy.start()
    return copy


def joined(rows, k):
    return jnp.concatenate([rows[k, 0], rows[k, 1]], axis=1)


def hidden_kernel(block, *refs):
    pieces, (scale, mine, theirs, out, rows, weights, row_sems, weight_sems) = refs[:-8], refs[-8:]
    chips = len(pieces)
    width = rows.shape[3]
    row_copies, weight_copies = [], {}
    for j, source in enumerate((mine, theirs)):
        for k in range(chips):
            if j == 0:
                row_copies.append(fetch(pieces[k], rows.at[k], row_sems.at[k]))
            for side in range(2):
                at = pl.multiple_of(block[2 * k + side] * width, width)
                weight_copies[j, k, side] = fetch(
                    source.at[pl.ds(at, width)],
                    weights.at[j, k, pl.ds(side * width, width)],
                    weight_sems.at[j, k, side],
                )
    half = out.shape[2]
    for j in range(2):
        acc = None
        for k in range(chips):
            if j == 0:
                row_copies[k].wait()
            for side in range(2):
                weight_copies[j, k, side].wait()
            part = jnp.dot(joined(rows, k), weights[j, k], preferred_element_type=F32)
            acc = part if acc is None else acc + part
        acc = acc * scale[:, :1]
        gate, up = acc[:, :half], acc[:, half:]
        out[j] = (gate / (1.0 + jnp.exp(-gate)) * up).astype(out.dtype)


def hidden_call(block, pieces, scale, mine, theirs):
    sides, count, width = pieces[0].shape
    chips = len(pieces)
    return pl.pallas_call(
        hidden_kernel,
        name="hidden",
        in_specs=[SCALARS] + [ANY] * chips + [WHOLE, ANY, ANY],
        out_specs=WHOLE,
        out_shape=jax.ShapeDtypeStruct((2, count, mine.shape[1] // 2), BF),
        scratch_shapes=[
            pltpu.VMEM((chips, sides, count, width), BF),
            pltpu.VMEM((2, chips, sides * width, mine.shape[1]), BF),
            pltpu.SemaphoreType.DMA((chips,)),
            pltpu.SemaphoreType.DMA((2, chips, 2)),
        ],
    )(block, *pieces, scale, mine, theirs)


def out_kernel(block, core, *refs):
    pieces, (mine, theirs, out, rows, weights, row_sems, weight_sems) = refs[:-7], refs[-7:]
    chips = len(pieces)
    width = rows.shape[3]
    cols = out.shape[2]
    row_copies, weight_copies = [], {}
    for k in range(chips):
        row_copies.append(fetch(pieces[k], rows.at[k], row_sems.at[k]))
        for side in range(2):
            at = pl.multiple_of(block[2 * k + side] * width, width)
            for j, source in enumerate((mine, theirs)):
                weight_copies[k, side, j] = fetch(
                    source.at[pl.ds(at, width)],
                    weights.at[k, pl.ds(side * width, width), pl.ds(j * cols, cols)],
                    weight_sems.at[k, side, j],
                )
    acc = None
    for k in range(chips):
        row_copies[k].wait()
        for side in range(2):
            for j in range(2):
                weight_copies[k, side, j].wait()
        part = jnp.dot(joined(rows, k), weights[k], preferred_element_type=F32)
        acc = part if acc is None else acc + part
    out[core[0]] = acc[:, :cols].astype(out.dtype)
    out[1 - core[0]] = acc[:, cols:].astype(out.dtype)


def out_call(block, core, pieces, mine, theirs):
    sides, count, width = pieces[0].shape
    chips, cols = len(pieces), mine.shape[1]
    return pl.pallas_call(
        out_kernel,
        name="expert_out",
        in_specs=[SCALARS, SCALARS] + [ANY] * (chips + 2),
        out_specs=WHOLE,
        out_shape=jax.ShapeDtypeStruct((2, count, cols), BF),
        scratch_shapes=[
            pltpu.VMEM((chips, sides, count, width), BF),
            pltpu.VMEM((chips, sides * width, 2 * cols), BF),
            pltpu.SemaphoreType.DMA((chips,)),
            pltpu.SemaphoreType.DMA((chips, 2, 2)),
        ],
        compiler_params=pltpu.CompilerParams(vmem_limit_bytes=20 * 1024 * 1024),
    )(block, core, *pieces, mine, theirs)


def cut_kernel(leaving, mine, theirs, *outs):
    width = outs[0].shape[1]
    for k, out in enumerate(outs):
        at = pl.multiple_of(leaving[k] * width, width)
        out[0] = mine[pl.ds(at, width), :]
        out[1] = theirs[pl.ds(at, width), :]


def cut_call(leaving, mine, theirs, width):
    count = leaving.shape[0]
    return pl.pallas_call(
        cut_kernel,
        name="cut",
        in_specs=[SCALARS, WHOLE, WHOLE],
        out_specs=[WHOLE] * count,
        out_shape=[jax.ShapeDtypeStruct((2, width, mine.shape[1]), BF)] * count,
        compiler_params=pltpu.CompilerParams(vmem_limit_bytes=12 * 1024 * 1024),
    )(leaving, mine, theirs)


def place_kernel(chip, core, *refs):
    pieces, out = refs[:-1], refs[-1]
    for k, piece in enumerate(pieces):

        @pl.when(pl.program_id(0) == k)
        def _(piece=piece):
            out[...] = jnp.concatenate([piece[core[0]], piece[1 - core[0]]], axis=1)


def place_call(chip, core, pieces):
    sides, rows, cols = pieces[0].shape
    chips = len(pieces)
    return pl.pallas_call(
        place_kernel,
        name="place",
        grid_spec=pltpu.PrefetchScalarGridSpec(
            num_scalar_prefetch=2,
            grid=(chips,),
            in_specs=[pl.BlockSpec((sides, rows, cols), lambda k, *_: (0, 0, 0))] * chips,
            out_specs=pl.BlockSpec((rows, sides * cols), lambda k, chip, core: (0, chip[k])),
        ),
        out_shape=jax.ShapeDtypeStruct((rows, chips * sides * cols), BF),
        compiler_params=pltpu.CompilerParams(vmem_limit_bytes=8 * 1024 * 1024),
    )(chip, core, *pieces)


def shift(value, by):
    count = lax.axis_size("x")
    return lax.ppermute(value, "x", [(i, (i + by) % count) for i in range(count)])


def swap(value):
    return lax.ppermute(value, "c", [(0, 1), (1, 0)])


def spread(value, offsets):
    return [shift(value, by) if by else value for by in offsets]


def exchange(value, axes):
    return lax.all_to_all(value, axes, split_axis=0, concat_axis=0, tiled=True)


def after(value, *others):
    return lax.optimization_barrier((value, *others))[0]


def both_groups(array):
    copies = jnp.broadcast_to(array[None], (lax.axis_size("gr"), *array.shape))
    return copies.reshape(-1, *array.shape[1:])


def body(prompt, norm_gain, gate_weight, up_weight, down_weight, routes, route_weight):
    experts, _, cols = gate_weight.shape
    tok_count, width = prompt.shape
    slots_all = experts * SLOTS
    half_all = slots_all // 2
    chips = lax.axis_size("x")
    chip, core = lax.axis_index("x"), lax.axis_index("c")
    offsets = [0, 1, chips - 1] + list(range(2, chips - 1))
    senders = [(chip - by) % chips for by in offsets]
    units = jnp.stack([2 * at + side for at in senders for side in (core, 1 - core)])
    units = units.astype(jnp.int32)
    core_id = core.reshape(1).astype(jnp.int32)

    expert_ids = jnp.arange(experts, dtype=jnp.int32)[None, :]
    first = routes[:, 0:1] == expert_ids
    second = routes[:, 1:2] == expert_ids
    named = (first | second).astype(BF)
    order = jnp.arange(tok_count, dtype=jnp.int32)
    before = (order[None, :] < order[:, None]).astype(BF)
    earlier = jnp.dot(before, named, preferred_element_type=F32)
    slot_first = jnp.sum(jnp.where(first, earlier, 0.0), axis=1).astype(jnp.int32)
    slot_second = jnp.sum(jnp.where(second, earlier, 0.0), axis=1).astype(jnp.int32)

    slot_ids = jnp.arange(slots_all, dtype=jnp.int32)[None, :]

    def picks(place):
        at_first = place(routes[:, 0], slot_first)[:, None] == slot_ids
        return at_first, place(routes[:, 1], slot_second)[:, None] == slot_ids

    is_first, is_second = picks(lambda expert, slot: expert * SLOTS + slot)
    outbound = jnp.einsum(
        "ts,td->sd", (is_first | is_second).astype(BF), prompt, preferred_element_type=F32
    ).astype(BF)
    moved = exchange(outbound.reshape(experts, SLOTS, width), "fs")
    halves = moved.reshape(experts, 2, HALF, width)
    mine, theirs = (
        lax.dynamic_slice_in_dim(halves, at, 1, 1).reshape(half_all, width)
        for at in (core, 1 - core)
    )
    arrived = spread(jnp.stack([mine, swap(theirs)]), offsets)
    is_first, is_second = picks(
        lambda expert, slot: slot // HALF * half_all + expert * HALF + slot % HALF
    )
    weighted = jnp.where(
        is_first, route_weight[:, 0:1], jnp.where(is_second, route_weight[:, 1:2], 0.0)
    ).astype(BF)
    scale = row_scale(arrived)

    gain = norm_gain[None, :, None]
    gate_up = jnp.concatenate(
        [(gate_weight * gain).astype(BF), (up_weight * gain).astype(BF)], axis=2
    )
    gate_up = both_groups(gate_up)
    gate_up = after(gate_up, moved)
    gate_up = exchange(gate_up, ("gr", "fs"))
    gate_up = gate_up.reshape(-1, 2 * cols)
    gate_up_other = swap(gate_up)
    gate_new, up_new = gate_up[None, :, :cols], gate_up[None, :, cols:]

    down = both_groups(down_weight.astype(BF))
    down = after(down, gate_up)
    down = exchange(down, ("gr", "fs"))
    down = down.reshape(-1, cols)
    down_other = swap(down)

    hidden = hidden_call(units, arrived, scale, gate_up, gate_up_other)
    hidden_all = spread(hidden, offsets)
    far = chips // 2
    near = [by for by in range(chips) if by != far]
    leaving = jnp.stack([2 * ((chip + by) % chips) + core for by in [far, *near]])
    leaving = leaving.astype(jnp.int32)
    blocks = {far: cut_call(leaving[:1], down, down_other, cols)[0]}
    blocks[far] = shift(blocks[far], far)
    summed = out_call(units, core_id, hidden_all, down, down_other)

    returned = exchange(summed.reshape(2 * experts, HALF, width), ("c", "fs"))
    returned = returned.reshape(slots_all, width)
    cut = cut_call(after(leaving[1:], summed), down, down_other, cols)
    for by, value in zip(near, cut):
        blocks[by] = shift(value, by) if by else value
    pieces = [blocks[by] for by in range(chips)]
    places = jnp.stack([(chip - by) % chips for by in range(chips)]).astype(jnp.int32)
    down_new = place_call(places, core_id, pieces)

    mixed = jnp.dot(weighted, returned, preferred_element_type=F32)
    return (gate_new, up_new, down_new[None], mixed.astype(BF))


def solution(mesh):
    groups, servers, shards = mesh.devices.shape
    devices = mesh.devices.reshape(groups, servers, shards // 2, 2)
    tp = ("x", "c")
    return jax.shard_map(
        body,
        mesh=Mesh(devices, ("gr", "fs", "x", "c")),
        in_specs=(
            P(("gr", "fs"), tp),
            P(("gr", "fs")),
            P(None, ("gr", "fs"), tp),
            P(None, ("gr", "fs"), tp),
            P(None, ("gr", "fs"), tp),
            P(("gr", "fs"), None),
            P(("gr", "fs"), None),
        ),
        out_specs=(
            P("fs", None, tp),
            P("fs", None, tp),
            P("fs", tp, None),
            P(("gr", "fs"), tp),
        ),
        check_vma=False,
    )
```
